512 devices in a mesh: grp: 2 (over y), sp: 32 (over z), tp: 8 (over x, core).
Axes of the slice: x: 4, y: 2, z: 32, core: 2. Of those that a mesh axis runs over, the one named last changes fastest.
The devices are a block of a 4x8x32 slice.
Arguments:
- prompt: bfloat16 [8, 6144, 2048], P('grp', 'sp'), parts along dimension 0, may hold values from -6 to 6
- w_key: bfloat16 [2048, 2048], P('sp', 'tp'), may hold values from -0.125 to 0.125
- w_value: bfloat16 [2048, 2048], P('sp', 'tp'), may hold values from -0.125 to 0.125
- query_new: bfloat16 [8, 2048], P('grp', 'tp'), parts along dimension 0, may hold values from -150 to 150
- key_new: bfloat16 [8, 2048], P('grp', 'tp'), parts along dimension 0, may hold values from -15 to 15
- value_new: bfloat16 [8, 2048], P('grp', 'tp'), parts along dimension 0, may hold values from -6 to 6
- mix_lambda: float32 [16], P('tp'), may hold values from 0.3 to 0.8
- head_gain: float32 [128], replicated, may hold values from 0.1 to 1.9
Outputs:
- key_cache: bfloat16 [64, 32, 24, 2048], P(('grp', 'sp'), None, None, 'tp'), parts along dimension 0
- value_cache: bfloat16 [64, 32, 24, 2048], P(('grp', 'sp'), None, None, 'tp'), parts along dimension 0
- first_read: bfloat16 [8, 2048], P('grp', 'tp'), parts along dimension 0
The draws below stay inside these ranges and needn't reach their ends.
There are 2 independent parts, one for each index of `grp`. The reference program is written for one: setup_inputs(seed, part) draws one part's arguments, and reference() takes and returns one part's arrays. A program takes and returns all parts, laid end to end along the dimension named above; an argument that names none is the same for every part. Nothing has to cross between parts.
All inputs are finite; a program needn't handle non-finite values.
Results may differ from the reference program's by a relative error of at most 0.0065.
The reference program's roundings to bfloat16 on the way (of `keys`, `values` and `mixed`) count: a program that leaves them out, or rounds other values in their place, can miss the bound.
Values may be sent and summed in bfloat16 or wider, within the bound.
No kernel may reach another device: no remote copies, remote signals or barrier semaphores. Data moves between devices by JAX's collectives and lax.ppermute only.
A program may use at most 64 MiB of HBM per device.

```python
import jax
import jax.numpy as jnp
from jax import lax

D = 2048
HEADS = 16
HALF = 64
VDIM = 128
SEQS = 4
LEN = 6144
N_SP = 32


def draw_query_new(key, part):
    base = jax.random.normal(key, (SEQS, HEADS, 2 * HALF), jnp.float32) * 1.75
    return jnp.clip(base, -10.0, 10.0).reshape(SEQS, HEADS * 2 * HALF).astype(jnp.bfloat16)


def levels(own_key, extent, pieces, least, high):
    def one(position, blocks):
        steps = jax.random.uniform(jax.random.fold_in(jax.random.fold_in(own_key, 6), position), (blocks,), jnp.float32, least / len(pieces), high / len(pieces))
        return jnp.repeat(jnp.exp(steps), extent[position] // blocks).reshape((-1,) + (1,) * (len(extent) - position - 1))

    gain = one(*pieces[0])
    for cut in pieces[1:]:
        gain = gain * one(*cut)
    return gain


def scatter_about(stream_key, shape, width, limit, cuts=(), kind=jnp.bfloat16):
    array = jax.random.normal(stream_key, shape, jnp.float32) * width
    if len(cuts) > 0:
        array = levels(stream_key, shape, cuts, -0.22, 0.18) * array
    return jnp.clip(array, min=-limit, max=limit).astype(kind)


def setup_inputs(seed: int = 0, part: int = 0) -> dict:
    seeds = jax.random.split(jax.random.key(seed), 9)
    own_keys = jax.random.split(jax.random.fold_in(seeds[8], part), 9)
    return {
        "prompt": scatter_about(own_keys[0], (SEQS, LEN, D), 1.0, 6.0, ((1, 32),)),
        "w_key": scatter_about(seeds[1], (D, HEADS * 2 * HALF), D ** -0.5, 0.125, ((0, 32), (1, 8))),
        "w_value": scatter_about(seeds[2], (D, HEADS * VDIM), D ** -0.5, 0.125, ((0, 32), (1, 8))),
        "query_new": draw_query_new(jax.random.fold_in(jax.random.fold_in(seeds[8], part), 71), part),
        "key_new": scatter_about(own_keys[4], (SEQS, HEADS * 2 * HALF), 2.5, 15.0, ((1, 8),)),
        "value_new": scatter_about(own_keys[5], (SEQS, HEADS * VDIM), 1.0, 6.0, ((1, 8),)),
        "mix_lambda": jnp.clip(0.3 + 0.5 * jax.random.uniform(seeds[6], (HEADS,), jnp.float32) ** levels(seeds[6], (HEADS,), ((0, 8),), -0.2, 0.2), 0.3, 0.8),
        "head_gain": jnp.clip(1.0 + 0.18 * jax.random.normal(seeds[7], (VDIM,), jnp.float32), 0.1, 1.9),
    }


def reference(prompt, w_key, w_value, query_new, key_new, value_new, mix_lambda, head_gain):
    rows = prompt.reshape(SEQS * LEN, D)
    keys = jnp.dot(rows, w_key, preferred_element_type=jnp.float32).astype(jnp.bfloat16)
    values = jnp.dot(rows, w_value, preferred_element_type=jnp.float32).astype(jnp.bfloat16)
    keys = keys.reshape(SEQS, LEN, HEADS * 2 * HALF)
    values = values.reshape(SEQS, LEN, HEADS * VDIM)
    scale = HALF ** (-0.5)

    def one_prompt(args):
        query, fresh_key, fresh_value, cached_keys, cached_values = args
        q_parts = query.astype(jnp.float32).reshape(HEADS, 2, HALF)
        k_parts = cached_keys.astype(jnp.float32).reshape(LEN, HEADS, 2, HALF)
        scores = jnp.einsum('hmc,lhmc->hml', q_parts, k_parts) * scale
        fresh = lax.optimization_barrier(jnp.sum(q_parts * fresh_key.astype(jnp.float32).reshape(HEADS, 2, HALF), axis=-1)) * scale
        top = jnp.maximum(lax.optimization_barrier(jnp.max(scores, axis=-1)), fresh)
        weights = jnp.exp(scores - top[..., None])
        own = jnp.exp(fresh - top)
        total = lax.optimization_barrier(jnp.sum(weights, axis=-1)) + own
        probs = weights / total[..., None]
        own_prob = own / total
        mixed = (probs[:, 0] - mix_lambda[:, None] * probs[:, 1]).astype(jnp.bfloat16)
        own_mixed = (own_prob[:, 0] - mix_lambda * own_prob[:, 1]).astype(jnp.bfloat16)
        value_parts = cached_values.astype(jnp.float32).reshape(LEN, HEADS, VDIM)
        reads = jnp.einsum('hl,lhv->hv', mixed.astype(jnp.float32), value_parts)
        reads = reads + own_mixed.astype(jnp.float32)[:, None] * fresh_value.astype(jnp.float32).reshape(HEADS, VDIM)
        mean = lax.optimization_barrier(jnp.mean(reads * reads, axis=-1, keepdims=True))
        normed = reads * lax.rsqrt(mean + 1e-06) * head_gain
        return normed.reshape(HEADS * VDIM).astype(jnp.bfloat16)
    first_read = lax.map(one_prompt, (query_new, key_new, value_new, keys, values))
    group = N_SP // SEQS
    sub = LEN // N_SP // group
    key_cache = keys.reshape(SEQS, N_SP, group, sub, HEADS * 2 * HALF).transpose(0, 2, 1, 3, 4)
    key_cache = key_cache.reshape(SEQS * group, N_SP, sub, HEADS * 2 * HALF)
    value_cache = values.reshape(SEQS, N_SP, group, sub, HEADS * VDIM).transpose(0, 2, 1, 3, 4)
    value_cache = value_cache.reshape(SEQS * group, N_SP, sub, HEADS * VDIM)
    return (key_cache, value_cache, first_read)
```

```python
import functools
import jax
import jax.numpy as jnp
from jax import lax
from jax.experimental import pallas as pl
from jax.experimental.pallas import tpu as pltpu
from jax.sharding import PartitionSpec as P

HALF = 64
VDIM = 128
W_SHIFT = 2.0**18
X_SHIFT = 2.0**13
F32 = jnp.float32
BF16 = jnp.bfloat16
NEG = -1e30


def row_dot(a, b, precision=None):
    return lax.dot_general(a, b, (((1,), (1,)), ((), ())), preferred_element_type=F32, precision=precision)


def select_rows(rows, query, count, heads, pairs):
    width = query.shape[1]
    r = lax.broadcasted_iota(jnp.int32, (rows, width), 0)
    lane = lax.broadcasted_iota(jnp.int32, (rows, width), 1)
    out = jnp.zeros((rows, width), F32)
    for b in range(count):
        q = jnp.broadcast_to(query[b : b + 1, :].astype(F32), (rows, width))
        out = jnp.where((r // heads) % count == b, q, out)
    slot = (r % heads) * pairs + r // (count * heads)
    return jnp.where(lane // HALF == slot, out, 0.0)


def local_kernel(peers, heads, x_ref, w_ref, q_ref, scores_ref, v_ref, stats_ref):
    count, piece, width = x_ref.shape
    rows = 2 * count * heads
    cols = heads * 2 * HALF
    x = x_ref[...].reshape(count * piece, width)
    keys = jnp.dot(x, w_ref[:, :cols], preferred_element_type=F32).astype(BF16)
    v_ref[...] = jnp.dot(x, w_ref[:, cols:], preferred_element_type=F32).astype(BF16)
    picked = select_rows(rows, q_ref[...], count, heads, 2)
    scores = row_dot(picked.astype(BF16), keys) * HALF**-0.5
    r = lax.broadcasted_iota(jnp.int32, scores.shape, 0)
    at = lax.broadcasted_iota(jnp.int32, scores.shape, 1)
    scores = jnp.where((r // heads) % count == at // piece, scores, NEG)
    scores_ref[...] = scores
    top = jnp.max(scores, axis=1, keepdims=True)
    total = jnp.sum(jnp.exp(scores - top), axis=1, keepdims=True)
    both = jnp.concatenate([top, total, jnp.zeros((128 - 2 * rows, 1), F32)], axis=0)
    stats_ref[...] = jnp.broadcast_to(both, (128, 128)).T[:peers]


def merged(stats, query, fresh_key, count, heads):
    rows = 2 * count * heads
    by_row = stats.T
    tops = by_row[:rows]
    totals = by_row[rows : 2 * rows]
    fresh = select_rows(rows, query, count, heads, 2) * select_rows(rows, fresh_key, count, heads, 2)
    fresh = jnp.sum(fresh, axis=1, keepdims=True) * HALF**-0.5
    top = jnp.maximum(jnp.max(tops, axis=1, keepdims=True), fresh)
    own = jnp.exp(fresh - top)
    total = jnp.sum(totals * jnp.exp(tops - top), axis=1, keepdims=True) + own
    return top, total, own


def per_row(lam_ref, rows, heads):
    r = lax.broadcasted_iota(jnp.int32, (rows, 1), 0) % heads
    out = jnp.zeros((rows, 1), F32)
    for h in range(heads):
        out = jnp.where(r == h, lam_ref[h], out)
    return out


def read_kernel(peers, heads, lam_ref, scores_ref, v_ref, stats_ref, q_ref, kn_ref, part_ref, own_ref):
    count = q_ref.shape[0]
    half = count * heads
    top, total, own = merged(stats_ref[...], q_ref[...], kn_ref[...], count, heads)
    probs = jnp.exp(scores_ref[...] - top) / total
    lam = per_row(lam_ref, half, heads)
    mixed = (probs[:half] - lam * probs[half:]).astype(BF16)
    full = jnp.dot(mixed, v_ref[...], preferred_element_type=F32)
    r = lax.broadcasted_iota(jnp.int32, (half, VDIM), 0)
    part = jnp.zeros((half, VDIM), F32)
    for h in range(heads):
        part = jnp.where(r % heads == h, full[:, h * VDIM : (h + 1) * VDIM], part)
    for p in range(peers):
        part_ref[p] = part
    prob = own / total
    mine = (prob[:half] - lam * prob[half:]).astype(BF16).astype(F32)
    own_ref[...] = jnp.broadcast_to(mine, (half, VDIM))


def finish_kernel(heads, parts_ref, own_ref, vn_ref, gain_ref, out_ref):
    count = vn_ref.shape[0]
    half = count * heads
    reads = jnp.sum(parts_ref[...], axis=0)
    values = vn_ref[...].astype(F32)
    r = lax.broadcasted_iota(jnp.int32, (half, VDIM), 0)
    fresh = jnp.zeros((half, VDIM), F32)
    for b in range(count):
        for h in range(heads):
            row = jnp.broadcast_to(values[b : b + 1, h * VDIM : (h + 1) * VDIM], (half, VDIM))
            fresh = jnp.where(r == b * heads + h, row, fresh)
    reads = reads + own_ref[...] * fresh
    mean = jnp.mean(reads * reads, axis=1, keepdims=True)
    normed = reads * lax.rsqrt(mean + 1e-06) * gain_ref[...]
    for b in range(count):
        for h in range(heads):
            out_ref[b : b + 1, h * VDIM : (h + 1) * VDIM] = normed[b * heads + h : b * heads + h + 1].astype(BF16)


def block_kernel(x_ref, w_ref, k_ref, v_ref):
    slices, rows, depth = x_ref.shape
    cols = k_ref.shape[1]
    acc = jnp.zeros((rows, 2 * cols), F32)
    for t in range(slices):
        acc += jnp.dot(x_ref[t], w_ref[t * depth : (t + 1) * depth, :], preferred_element_type=F32)
    k_ref[...] = acc[:, :cols].astype(BF16)
    v_ref[...] = acc[:, cols:].astype(BF16)


def vmem(n):
    return [pl.BlockSpec(memory_space=pltpu.VMEM)] * n


def call(kernel, outs, args, smem=0):
    specs = [pl.BlockSpec(memory_space=pltpu.SMEM)] * smem + vmem(len(args) - smem)
    return pl.pallas_call(
        kernel,
        out_shape=[jax.ShapeDtypeStruct(s, d) for s, d in outs],
        in_specs=specs,
        out_specs=vmem(len(outs)),
        compiler_params=pltpu.CompilerParams(vmem_limit_bytes=40 << 20),
    )(*args)


def spread(x, axis):
    return lax.all_to_all(x, axis, 0, 0, tiled=True)


def body(prompt, w_key, w_value, query_new, key_new, value_new, mix_lambda, head_gain):
    count, piece, width = prompt.shape
    peers = lax.axis_size("sp")
    slices = lax.axis_size("tp")
    groups = peers // count
    sub = piece // groups
    heads = mix_lambda.shape[0]
    cols = w_key.shape[1]
    half = count * heads

    depth = width // slices
    mine = lax.dynamic_slice_in_dim(prompt, lax.axis_index("tp") * depth, depth, 2)
    mine = (mine.astype(F32) * X_SHIFT).astype(jnp.float16).reshape(peers, sub, depth)

    w = jnp.concatenate([w_key, w_value], axis=1)
    w = (w.astype(F32) * W_SHIFT).astype(jnp.float16)
    w = lax.all_gather(w, "sp", axis=0, tiled=True)
    w, mine = lax.optimization_barrier((w, mine))
    blocks = spread(mine, "sp")
    w = (w.astype(F32) * (1 / W_SHIFT)).astype(BF16)

    scores, values, stats = call(
        functools.partial(local_kernel, peers, heads),
        [((2 * half, count * piece), F32), ((count * piece, cols), BF16), ((peers, 128), F32)],
        (prompt, w, query_new),
    )
    stats = spread(stats, "sp")
    parts, own = call(
        functools.partial(read_kernel, peers, heads),
        [((peers, half, VDIM), F32), ((half, VDIM), F32)],
        (mix_lambda, scores, values, stats, query_new, key_new),
        smem=1,
    )
    parts = spread(parts, "sp")
    (first_read,) = call(
        functools.partial(finish_kernel, heads),
        [((count, cols), BF16)],
        (parts, own, value_new, head_gain.reshape(1, VDIM)),
    )

    blocks = lax.all_gather(blocks.reshape(peers * sub, depth), "tp", axis=0)
    blocks = (blocks.astype(F32) * (1 / X_SHIFT)).astype(BF16)
    key_cache, value_cache = call(
        block_kernel,
        [((peers * sub, cols), BF16)] * 2,
        (blocks, w),
    )
    shape = (1, peers, sub, cols)
    return key_cache.reshape(shape), value_cache.reshape(shape), first_read


def solution(mesh):
    return jax.shard_map(
        body,
        mesh=mesh,
        in_specs=(
            P("grp", "sp", None),
            P("sp", "tp"),
            P("sp", "tp"),
            P("grp", "tp"),
            P("grp", "tp"),
            P("grp", "tp"),
            P("tp"),
            P(),
        ),
        out_specs=(
            P(("grp", "sp"), None, None, "tp"),
            P(("grp", "sp"), None, None, "tp"),
            P("grp", "tp"),
        ),
        check_vma=False,
    )
```

```python
import functools
import jax
import jax.numpy as jnp
from jax import lax
from jax.experimental import pallas as pl
from jax.experimental.pallas import tpu as pltpu
from jax.sharding import PartitionSpec as P

HALF = 64
VDIM = 128
W_SHIFT = 2.0**18
F32 = jnp.float32
BF16 = jnp.bfloat16
NEG = -1e30
LIMIT = 16


def row_dot(a, b, precision=None):
    return lax.dot_general(a, b, (((1,), (1,)), ((), ())), preferred_element_type=F32, precision=precision)


def select_rows(rows, query, count, heads, pairs):
    width = query.shape[1]
    r = lax.broadcasted_iota(jnp.int32, (rows, width), 0)
    lane = lax.broadcasted_iota(jnp.int32, (rows, width), 1)
    out = jnp.zeros((rows, width), F32)
    for b in range(count):
        q = jnp.broadcast_to(query[b : b + 1, :].astype(F32), (rows, width))
        out = jnp.where((r // heads) % count == b, q, out)
    slot = (r % heads) * pairs + r // (count * heads)
    return jnp.where(lane // HALF == slot, out, 0.0)


def local_kernel(peers, heads, x_ref, w_ref, q_ref, part_ref):
    count, piece, width = x_ref.shape
    rows = 2 * count * heads
    cols = heads * 2 * HALF
    x = x_ref[...].reshape(count * piece, width)
    keys = jnp.dot(x, w_ref[:, :cols], preferred_element_type=F32).astype(BF16)
    values = jnp.dot(x, w_ref[:, cols:], preferred_element_type=F32).astype(BF16)
    picked = select_rows(rows, q_ref[...], count, heads, 2)
    scores = row_dot(picked.astype(BF16), keys) * HALF**-0.5
    r = lax.broadcasted_iota(jnp.int32, scores.shape, 0)
    at = lax.broadcasted_iota(jnp.int32, scores.shape, 1)
    scores = jnp.where((r // heads) % count == at // piece, scores, NEG)
    top = jnp.max(scores, axis=1, keepdims=True)
    weights = jnp.exp(scores - top)
    total = jnp.sum(weights, axis=1, keepdims=True)
    full = 0.0
    for p in three(weights):
        full += jnp.dot(p, values, preferred_element_type=F32)
    r = lax.broadcasted_iota(jnp.int32, (rows, VDIM), 0)
    part = jnp.zeros((rows, VDIM), F32)
    for h in range(heads):
        part = jnp.where(r % heads == h, full[:, h * VDIM : (h + 1) * VDIM], part)
    stats = as_line([top, total])
    for p in range(peers):
        part_ref[p * (rows + 1) : p * (rows + 1) + rows, :] = part
        part_ref[p * (rows + 1) + rows : (p + 1) * (rows + 1), :] = stats


def three(x):
    high = x.astype(BF16)
    rest = x - high.astype(F32)
    middle = rest.astype(BF16)
    return high, middle, (rest - middle.astype(F32)).astype(BF16)


def as_line(columns):
    rows = sum(c.shape[0] for c in columns)
    both = jnp.concatenate([*columns, jnp.zeros((VDIM - rows, 1), F32)], axis=0)
    return jnp.broadcast_to(both, (VDIM, VDIM)).T[:1]


def finish_kernel(peers, heads, lam_ref, part_ref, q_ref, kn_ref, vn_ref, gain_ref, out_ref):
    count = vn_ref.shape[0]
    half = count * heads
    rows = 2 * half
    fresh = select_rows(rows, q_ref[...], count, heads, 2) * select_rows(rows, kn_ref[...], count, heads, 2)
    fresh = as_line([jnp.sum(fresh, axis=1, keepdims=True) * HALF**-0.5])
    tops = part_ref[pl.ds(rows, peers, rows + 1), :]
    totals = pltpu.roll(tops, VDIM - rows, 1)
    top = jnp.maximum(jnp.max(tops, axis=0, keepdims=True), fresh)
    scale = jnp.exp(tops - top)
    own = jnp.exp(fresh - top)
    total = jnp.sum(totals * scale, axis=0, keepdims=True) + own
    lane = lax.broadcasted_iota(jnp.int32, (1, VDIM), 1)
    sign = jnp.ones((1, VDIM), F32)
    for h in range(heads):
        sign = jnp.where((lane >= half) & (lane % heads == h), -lam_ref[h], sign)
    scale = scale * (sign / total)
    own = own * (sign / total)
    mine = (own + pltpu.roll(own, VDIM - half, 1)).astype(BF16).astype(F32)
    values = vn_ref[...].astype(F32)
    for b in range(count):
        for h in range(heads):
            n = b * heads + h
            reads = 0.0
            for r in (n, n + half):
                reads += scale[:, r : r + 1] * part_ref[pl.ds(r, peers, rows + 1), :]
            reads = jnp.sum(reads, axis=0, keepdims=True)
            reads += mine[:, n : n + 1] * values[b : b + 1, h * VDIM : (h + 1) * VDIM]
            mean = jnp.mean(reads * reads, axis=1, keepdims=True)
            normed = reads * lax.rsqrt(mean + 1e-06) * gain_ref[...]
            out_ref[b : b + 1, h * VDIM : (h + 1) * VDIM] = normed.astype(BF16)


def block_kernel(slices, t_ref, *refs):
    x_refs, (w_ref, k_ref, v_ref, w_buf, sem) = refs[:slices], refs[slices:]
    rows, depth = x_refs[0].shape
    cols = k_ref.shape[1]
    moves = []
    for n in range(slices):
        w = pl.ds(pl.multiple_of(t_ref[n] * depth, depth), depth)
        moves.append(pltpu.make_async_copy(w_ref.at[w, :], w_buf.at[n], sem.at[n]))
        moves[n].start()
    step = rows // 4
    for at in range(0, rows, step):
        acc = 0.0
        for n in range(slices):
            if at == 0:
                moves[n].wait()
            acc += jnp.dot(x_refs[n][at : at + step, :], w_buf[n], preferred_element_type=F32)
        k_ref[at : at + step, :] = acc[:, :cols].astype(BF16)
        v_ref[at : at + step, :] = acc[:, cols:].astype(BF16)


def vmem(n):
    return [pl.BlockSpec(memory_space=pltpu.VMEM)] * n


def call(kernel, outs, args, spaces="", scratch=(), limit=16):
    kinds = {"s": pltpu.SMEM, "a": pl.ANY, "v": pltpu.VMEM}
    spaces = spaces.ljust(len(args), "v")
    return pl.pallas_call(
        kernel,
        out_shape=[jax.ShapeDtypeStruct(s, d) for s, d in outs],
        in_specs=[pl.BlockSpec(memory_space=kinds[c]) for c in spaces],
        out_specs=vmem(len(outs)),
        scratch_shapes=scratch,
        compiler_params=pltpu.CompilerParams(vmem_limit_bytes=int(limit * 2**20)),
    )(*args)


def spread(x, axis):
    return lax.all_to_all(x, axis, 0, 0, tiled=True)


def moved(x, axis, step):
    n = lax.axis_size(axis)
    return lax.ppermute(x, axis, [(i, step(i) % n) for i in range(n)])


def inner(prompt, w_key, w_value, query_new, key_new, value_new, mix_lambda, head_gain):
    count, piece, width = prompt.shape
    peers = lax.axis_size("sp")
    slices = lax.axis_size("tp")
    groups = peers // count
    sub = piece // groups
    heads = mix_lambda.shape[0]
    cols = w_key.shape[1]
    half = count * heads
    t = lax.axis_index("tp")

    depth = width // slices
    mine = lax.dynamic_slice_in_dim(prompt, t * depth, depth, 2).reshape(peers, sub, depth)
    w = jnp.concatenate([w_key, w_value], axis=1)
    w = (w.astype(F32) * W_SHIFT).astype(jnp.float16)
    mine, w = lax.optimization_barrier((mine, w))
    w = lax.all_gather(w, "sp", axis=0, tiled=True)
    w, mine = lax.optimization_barrier((w, mine))
    mine = spread(mine, "sp").reshape(peers * sub, depth)
    w = (w.astype(F32) * (1 / W_SHIFT)).astype(BF16)

    (parts,) = call(
        functools.partial(local_kernel, peers, heads), [((peers * (2 * half + 1), VDIM), F32)], (prompt, w, query_new)
    )
    parts = parts.reshape(peers, 1, (2 * half + 1) * VDIM)
    parts = spread(parts, "sp").reshape(peers * (2 * half + 1), VDIM)
    (first_read,) = call(
        functools.partial(finish_kernel, peers, heads),
        [((count, cols), BF16)],
        (mix_lambda, parts, query_new, key_new, value_new, head_gain.reshape(1, VDIM)),
        "s",
    )

    found, who = [mine], [t]
    for d in range(1, slices // 2):
        found.append(moved(mine, "tp", lambda i: i + 2 * d))
        who.append((t - 2 * d) % slices)
    for n in range(slices // 2):
        found.append(moved(found[n], "tp", lambda i: i ^ 1))
        who.append(who[n] ^ 1)
    key_cache, value_cache = call(
        functools.partial(block_kernel, slices),
        [((peers * sub, cols), BF16)] * 2,
        (jnp.stack(who), *found, w),
        "s" + "v" * slices + "a",
        [pltpu.VMEM((slices, depth, 2 * cols), BF16), pltpu.SemaphoreType.DMA((slices,))],
        LIMIT,
    )
    shape = (1, peers, sub, cols)
    return key_cache.reshape(shape), value_cache.reshape(shape), first_read


def solution(mesh):
    return jax.shard_map(
        inner,
        mesh=mesh,
        in_specs=(
            P("grp", "sp", None),
            P("sp", "tp"),
            P("sp", "tp"),
            P("grp", "tp"),
            P("grp", "tp"),
            P("grp", "tp"),
            P("tp"),
            P(),
        ),
        out_specs=(
            P(("grp", "sp"), None, None, "tp"),
            P(("grp", "sp"), None, None, "tp"),
            P("grp", "tp"),
        ),
        check_vma=False,
    )
```

```python
import functools
import jax
import jax.numpy as jnp
from jax import lax
from jax.experimental import pallas as pl
from jax.experimental.pallas import tpu as pltpu
from jax.sharding import PartitionSpec as P

HALF = 64
VDIM = 128
W_SHIFT = 2.0**18
F32 = jnp.float32
BF16 = jnp.bfloat16
NEG = -1e30
LIMIT = 16


def row_dot(a, b, precision=None):
    return lax.dot_general(a, b, (((1,), (1,)), ((), ())), preferred_element_type=F32, precision=precision)


def select_rows(rows, query, count, heads, pairs):
    width = query.shape[1]
    r = lax.broadcasted_iota(jnp.int32, (rows, width), 0)
    lane = lax.broadcasted_iota(jnp.int32, (rows, width), 1)
    out = jnp.zeros((rows, width), F32)
    for b in range(count):
        q = jnp.broadcast_to(query[b : b + 1, :].astype(F32), (rows, width))
        out = jnp.where((r // heads) % count == b, q, out)
    slot = (r % heads) * pairs + r // (count * heads)
    return jnp.where(lane // HALF == slot, out, 0.0)


def local_kernel(peers, heads, x_ref, w_ref, q_ref, part_ref):
    count, piece, width = x_ref.shape
    rows = 2 * count * heads
    cols = heads * 2 * HALF
    x = x_ref[...].reshape(count * piece, width)
    keys = jnp.dot(x, w_ref[:, :cols], preferred_element_type=F32).astype(BF16)
    values = jnp.dot(x, w_ref[:, cols:], preferred_element_type=F32).astype(BF16)
    picked = select_rows(rows, q_ref[...], count, heads, 2)
    scores = row_dot(picked.astype(BF16), keys) * HALF**-0.5
    r = lax.broadcasted_iota(jnp.int32, scores.shape, 0)
    at = lax.broadcasted_iota(jnp.int32, scores.shape, 1)
    scores = jnp.where((r // heads) % count == at // piece, scores, NEG)
    top = jnp.max(scores, axis=1, keepdims=True)
    weights = jnp.exp(scores - top)
    total = jnp.sum(weights, axis=1, keepdims=True)
    full = 0.0
    for p in three(weights):
        full += jnp.dot(p, values, preferred_element_type=F32)
    r = lax.broadcasted_iota(jnp.int32, (rows, VDIM), 0)
    part = jnp.zeros((rows, VDIM), F32)
    for h in range(heads):
        part = jnp.where(r % heads == h, full[:, h * VDIM : (h + 1) * VDIM], part)
    stats = as_line([top, total])
    for p in range(peers):
        part_ref[p * (rows + 1) : p * (rows + 1) + rows, :] = part
        part_ref[p * (rows + 1) + rows : (p + 1) * (rows + 1), :] = stats


def three(x):
    high = x.astype(BF16)
    rest = x - high.astype(F32)
    middle = rest.astype(BF16)
    return high, middle, (rest - middle.astype(F32)).astype(BF16)


def as_line(columns):
    rows = sum(c.shape[0] for c in columns)
    both = jnp.concatenate([*columns, jnp.zeros((VDIM - rows, 1), F32)], axis=0)
    return jnp.broadcast_to(both, (VDIM, VDIM)).T[:1]


def fresh_kernel(heads, lam_ref, q_ref, kn_ref, vn_ref, gain_ref, out_ref):
    count = vn_ref.shape[0]
    half = count * heads
    rows = 2 * half
    fresh = select_rows(rows, q_ref[...], count, heads, 2) * select_rows(rows, kn_ref[...], count, heads, 2)
    out_ref[0:1, :] = as_line([jnp.sum(fresh, axis=1, keepdims=True) * HALF**-0.5])
    lane = lax.broadcasted_iota(jnp.int32, (1, VDIM), 1)
    sign = jnp.ones((1, VDIM), F32)
    for h in range(heads):
        sign = jnp.where((lane >= half) & (lane % heads == h), -lam_ref[h], sign)
    out_ref[1:2, :] = sign
    out_ref[2:3, :] = gain_ref[...]
    out_ref[3:8, :] = jnp.zeros((5, VDIM), F32)
    values = vn_ref[...].astype(F32)
    for b in range(count):
        for h in range(heads):
            n = 8 + b * heads + h
            out_ref[n : n + 1, :] = values[b : b + 1, h * VDIM : (h + 1) * VDIM]


def finish_kernel(peers, heads, part_ref, new_ref, out_ref):
    count = out_ref.shape[0]
    half = count * heads
    rows = 2 * half
    fresh = new_ref[0:1, :]
    tops = part_ref[pl.ds(rows, peers, rows + 1), :]
    totals = pltpu.roll(tops, VDIM - rows, 1)
    top = jnp.maximum(jnp.max(tops, axis=0, keepdims=True), fresh)
    scale = jnp.exp(tops - top)
    own = jnp.exp(fresh - top)
    total = jnp.sum(totals * scale, axis=0, keepdims=True) + own
    scale = scale * (new_ref[1:2, :] / total)
    own = own * (new_ref[1:2, :] / total)
    mine = (own + pltpu.roll(own, VDIM - half, 1)).astype(BF16).astype(F32)
    for b in range(count):
        for h in range(heads):
            n = b * heads + h
            reads = 0.0
            for r in (n, n + half):
                reads += scale[:, r : r + 1] * part_ref[pl.ds(r, peers, rows + 1), :]
            reads = jnp.sum(reads, axis=0, keepdims=True)
            reads += mine[:, n : n + 1] * new_ref[8 + n : 9 + n, :]
            mean = jnp.mean(reads * reads, axis=1, keepdims=True)
            normed = reads * lax.rsqrt(mean + 1e-06) * new_ref[2:3, :]
            out_ref[b : b + 1, h * VDIM : (h + 1) * VDIM] = normed.astype(BF16)


def block_kernel(slices, *refs):
    x_refs, (w_ref, k_ref, v_ref, x_buf, w_buf, sem) = refs[:slices], refs[slices:]
    rows, depth = x_refs[0].shape
    cols = k_ref.shape[1]
    t = lax.axis_index("tp")
    who = [lax.rem(t + slices - 2 * d, slices) for d in range(slices // 2)]
    who += [lax.bitwise_xor(n, 1) for n in who]
    moves = []
    for n in range(slices):
        w = pl.ds(pl.multiple_of(who[n] * depth, depth), depth)
        moves.append(
            [
                pltpu.make_async_copy(w_ref.at[w, :], w_buf.at[n], sem.at[n, 0]),
                pltpu.make_async_copy(x_refs[n], x_buf.at[n], sem.at[n, 1]),
            ]
        )
        for m in moves[n]:
            m.start()
    step = rows // 4
    for at in range(0, rows, step):
        acc = 0.0
        for n in range(slices):
            if at == 0:
                for m in moves[n]:
                    m.wait()
            acc += jnp.dot(x_buf[n, at : at + step, :], w_buf[n], preferred_element_type=F32)
        k_ref[at : at + step, :] = acc[:, :cols].astype(BF16)
        v_ref[at : at + step, :] = acc[:, cols:].astype(BF16)


def call(kernel, outs, args, spaces="", scratch=(), limit=16):
    kinds = {"s": pltpu.SMEM, "a": pl.ANY, "v": pltpu.VMEM}
    spaces = spaces.ljust(len(args), "v")
    return pl.pallas_call(
        kernel,
        out_shape=[jax.ShapeDtypeStruct(s, d) for s, d in outs],
        in_specs=[pl.BlockSpec(memory_space=kinds[c]) for c in spaces],
        out_specs=[pl.BlockSpec(memory_space=pltpu.VMEM)] * len(outs),
        scratch_shapes=scratch,
        compiler_params=pltpu.CompilerParams(vmem_limit_bytes=int(limit * 2**20)),
    )(*args)


def spread(x, axis):
    return lax.all_to_all(x, axis, 0, 0, tiled=True)


def moved(x, axis, step):
    n = lax.axis_size(axis)
    return lax.ppermute(x, axis, [(i, step(i) % n) for i in range(n)])


def inner(prompt, w_key, w_value, query_new, key_new, value_new, mix_lambda, head_gain):
    count, piece, width = prompt.shape
    peers = lax.axis_size("sp")
    slices = lax.axis_size("tp")
    groups = peers // count
    sub = piece // groups
    heads = mix_lambda.shape[0]
    cols = w_key.shape[1]
    half = count * heads
    t = lax.axis_index("tp")

    depth = width // slices
    mine = lax.dynamic_slice_in_dim(prompt, t * depth, depth, 2).reshape(peers, sub, depth)
    w = jnp.concatenate([w_key, w_value], axis=1)
    w = (w.astype(F32) * W_SHIFT).astype(jnp.float16)
    mine, w = lax.optimization_barrier((mine, w))
    w = lax.all_gather(w, "sp", axis=0, tiled=True)
    w = (w.astype(F32) * (1 / W_SHIFT)).astype(BF16)
    w, mine = lax.optimization_barrier((w, mine))
    mine = spread(mine, "sp").reshape(peers * sub, depth)

    (fresh,) = call(
        functools.partial(fresh_kernel, heads),
        [((8 + half, VDIM), F32)],
        (mix_lambda, query_new, key_new, value_new, head_gain.reshape(1, VDIM)),
        "s",
    )
    (parts,) = call(
        functools.partial(local_kernel, peers, heads), [((peers * (2 * half + 1), VDIM), F32)], (prompt, w, query_new)
    )
    parts = parts.reshape(peers, 1, (2 * half + 1) * VDIM)
    parts = spread(parts, "sp").reshape(peers * (2 * half + 1), VDIM)
    (first_read,) = call(functools.partial(finish_kernel, peers, heads), [((count, cols), BF16)], (parts, fresh))

    found = [mine]
    for d in range(1, slices // 2):
        found.append(moved(mine, "tp", lambda i: i + 2 * d))
    for n in range(slices // 2):
        found.append(moved(found[n], "tp", lambda i: i ^ 1))
    key_cache, value_cache = call(
        functools.partial(block_kernel, slices),
        [((peers * sub, cols), BF16)] * 2,
        (*found, w),
        "a" * (slices + 1),
        [
            pltpu.VMEM((slices, peers * sub, depth), BF16),
            pltpu.VMEM((slices, depth, 2 * cols), BF16),
            pltpu.SemaphoreType.DMA((slices, 2)),
        ],
        LIMIT,
    )
    shape = (1, peers, sub, cols)
    return key_cache.reshape(shape), value_cache.reshape(shape), first_read


def solution(mesh):
    return jax.shard_map(
        inner,
        mesh=mesh,
        in_specs=(
            P("grp", "sp", None),
            P("sp", "tp"),
            P("sp", "tp"),
            P("grp", "tp"),
            P("grp", "tp"),
            P("grp", "tp"),
            P("tp"),
            P(),
        ),
        out_specs=(
            P(("grp", "sp"), None, None, "tp"),
            P(("grp", "sp"), None, None, "tp"),
            P("grp", "tp"),
        ),
        check_vma=False,
    )
```

```python
import functools
import jax
import jax.numpy as jnp
from jax import lax
from jax.experimental import pallas as pl
from jax.experimental.pallas import tpu as pltpu
from jax.sharding import PartitionSpec as P

HALF = 64
VDIM = 128
W_SHIFT = 2.0**18
F32 = jnp.float32
BF16 = jnp.bfloat16
NEG = -1e30
LIMIT = 16


def row_dot(a, b, precision=None):
    return lax.dot_general(a, b, (((1,), (1,)), ((), ())), preferred_element_type=F32, precision=precision)


def select_rows(rows, query, count, heads, pairs):
    width = query.shape[1]
    r = lax.broadcasted_iota(jnp.int32, (rows, width), 0)
    lane = lax.broadcasted_iota(jnp.int32, (rows, width), 1)
    out = jnp.zeros((rows, width), F32)
    for b in range(count):
        q = jnp.broadcast_to(query[b : b + 1, :].astype(F32), (rows, width))
        out = jnp.where((r // heads) % count == b, q, out)
    slot = (r % heads) * pairs + r // (count * heads)
    return jnp.where(lane // HALF == slot, out, 0.0)


def local_kernel(peers, heads, x_ref, w_ref, q_ref, part_ref):
    count, piece, width = x_ref.shape
    rows = 2 * count * heads
    cols = heads * 2 * HALF
    x = x_ref[...].reshape(count * piece, width)
    keys = jnp.dot(x, w_ref[:, :cols], preferred_element_type=F32).astype(BF16)
    values = jnp.dot(x, w_ref[:, cols:], preferred_element_type=F32).astype(BF16)
    picked = select_rows(rows, q_ref[...], count, heads, 2)
    scores = row_dot(picked.astype(BF16), keys) * HALF**-0.5
    r = lax.broadcasted_iota(jnp.int32, scores.shape, 0)
    at = lax.broadcasted_iota(jnp.int32, scores.shape, 1)
    scores = jnp.where((r // heads) % count == at // piece, scores, NEG)
    top = jnp.max(scores, axis=1, keepdims=True)
    weights = jnp.exp(scores - top)
    total = jnp.sum(weights, axis=1, keepdims=True)
    full = 0.0
    for p in three(weights):
        full += jnp.dot(p, values, preferred_element_type=F32)
    r = lax.broadcasted_iota(jnp.int32, (rows, VDIM), 0)
    part = jnp.zeros((rows, VDIM), F32)
    for h in range(heads):
        part = jnp.where(r % heads == h, full[:, h * VDIM : (h + 1) * VDIM], part)
    stats = as_line([top, total])
    for p in range(peers):
        part_ref[p * (rows + 1) : p * (rows + 1) + rows, :] = part
        part_ref[p * (rows + 1) + rows : (p + 1) * (rows + 1), :] = stats


def three(x):
    high = x.astype(BF16)
    rest = x - high.astype(F32)
    middle = rest.astype(BF16)
    return high, middle, (rest - middle.astype(F32)).astype(BF16)


def as_line(columns):
    rows = sum(c.shape[0] for c in columns)
    both = jnp.concatenate([*columns, jnp.zeros((VDIM - rows, 1), F32)], axis=0)
    return jnp.broadcast_to(both, (VDIM, VDIM)).T[:1]


def fresh_kernel(heads, lam_ref, met_ref, q_ref, kn_ref, vn_ref, gain_ref, out_ref):
    count = vn_ref.shape[0]
    half = count * heads
    rows = 2 * half
    fresh = select_rows(rows, q_ref[...], count, heads, 2) * select_rows(rows, kn_ref[...], count, heads, 2)
    out_ref[0:1, :] = as_line([jnp.sum(fresh, axis=1, keepdims=True) * HALF**-0.5])
    lane = lax.broadcasted_iota(jnp.int32, (1, VDIM), 1)
    sign = jnp.ones((1, VDIM), F32)
    for h in range(heads):
        sign = jnp.where((lane >= half) & (lane % heads == h), -lam_ref[h], sign)
    out_ref[1:2, :] = sign
    out_ref[2:3, :] = gain_ref[...]
    out_ref[3:8, :] = jnp.zeros((5, VDIM), F32)
    values = vn_ref[...].astype(F32)
    for b in range(count):
        for h in range(heads):
            n = 8 + b * heads + h
            out_ref[n : n + 1, :] = values[b : b + 1, h * VDIM : (h + 1) * VDIM]


def finish_kernel(peers, heads, part_ref, new_ref, out_ref):
    count = out_ref.shape[0]
    half = count * heads
    rows = 2 * half
    fresh = new_ref[0:1, :]
    tops = part_ref[pl.ds(rows, peers, rows + 1), :]
    totals = pltpu.roll(tops, VDIM - rows, 1)
    top = jnp.maximum(jnp.max(tops, axis=0, keepdims=True), fresh)
    scale = jnp.exp(tops - top)
    own = jnp.exp(fresh - top)
    total = jnp.sum(totals * scale, axis=0, keepdims=True) + own
    scale = scale * (new_ref[1:2, :] / total)
    own = own * (new_ref[1:2, :] / total)
    mine = (own + pltpu.roll(own, VDIM - half, 1)).astype(BF16).astype(F32)
    for b in range(count):
        for h in range(heads):
            n = b * heads + h
            reads = 0.0
            for r in (n, n + half):
                reads += scale[:, r : r + 1] * part_ref[pl.ds(r, peers, rows + 1), :]
            reads = jnp.sum(reads, axis=0, keepdims=True)
            reads += mine[:, n : n + 1] * new_ref[8 + n : 9 + n, :]
            mean = jnp.mean(reads * reads, axis=1, keepdims=True)
            normed = reads * lax.rsqrt(mean + 1e-06) * new_ref[2:3, :]
            out_ref[b : b + 1, h * VDIM : (h + 1) * VDIM] = normed.astype(BF16)


def block_kernel(slices, *refs):
    x_refs, (w_ref, k_ref, v_ref, x_buf, w_buf, sem) = refs[:slices], refs[slices:]
    rows, depth = x_refs[0].shape
    cols = k_ref.shape[1]
    t = lax.axis_index("tp")
    who = [lax.rem(t + slices - 2 * d, slices) for d in range(slices // 2)]
    who += [lax.bitwise_xor(n, 1) for n in who]
    moves = []
    for n in range(slices):
        w = pl.ds(pl.multiple_of(who[n] * depth, depth), depth)
        moves.append(
            [
                pltpu.make_async_copy(w_ref.at[w, :], w_buf.at[n], sem.at[n, 0]),
                pltpu.make_async_copy(x_refs[n], x_buf.at[n], sem.at[n, 1]),
            ]
        )
        for m in moves[n]:
            m.start()
    step = rows // 4
    for at in range(0, rows, step):
        acc = 0.0
        for n in range(slices):
            if at == 0:
                for m in moves[n]:
                    m.wait()
            acc += jnp.dot(x_buf[n, at : at + step, :], w_buf[n], preferred_element_type=F32)
        k_ref[at : at + step, :] = acc[:, :cols].astype(BF16)
        v_ref[at : at + step, :] = acc[:, cols:].astype(BF16)


def call(kernel, outs, args, spaces="", scratch=(), limit=16):
    kinds = {"s": pltpu.SMEM, "a": pl.ANY, "v": pltpu.VMEM}
    spaces = spaces.ljust(len(args), "v")
    return pl.pallas_call(
        kernel,
        out_shape=[jax.ShapeDtypeStruct(s, d) for s, d in outs],
        in_specs=[pl.BlockSpec(memory_space=kinds[c]) for c in spaces],
        out_specs=[pl.BlockSpec(memory_space=pltpu.VMEM)] * len(outs),
        scratch_shapes=scratch,
        compiler_params=pltpu.CompilerParams(vmem_limit_bytes=int(limit * 2**20)),
    )(*args)


def spread(x, axis):
    return lax.all_to_all(x, axis, 0, 0, tiled=True)


def moved(x, axis, step):
    n = lax.axis_size(axis)
    return lax.ppermute(x, axis, [(i, step(i) % n) for i in range(n)])


def inner(prompt, w_key, w_value, query_new, key_new, value_new, mix_lambda, head_gain):
    count, piece, width = prompt.shape
    peers = lax.axis_size("sp")
    slices = lax.axis_size("tp")
    groups = peers // count
    sub = piece // groups
    heads = mix_lambda.shape[0]
    cols = w_key.shape[1]
    half = count * heads
    t = lax.axis_index("tp")

    depth = width // slices
    mine = lax.dynamic_slice_in_dim(prompt, t * depth, depth, 2).reshape(peers, sub, depth)
    w = jnp.concatenate([w_key, w_value], axis=1)
    w = (w.astype(F32) * W_SHIFT).astype(jnp.float16)
    mine, w = lax.optimization_barrier((mine, w))
    w = lax.all_gather(w, "sp", axis=0, tiled=True)
    w = (w.astype(F32) * (1 / W_SHIFT)).astype(BF16)
    w, mine = lax.optimization_barrier((w, mine))
    met = moved(w[:8, :VDIM], "tp", lambda i: i ^ 1)
    mine = spread(mine, "sp").reshape(peers * sub, depth)

    (fresh,) = call(
        functools.partial(fresh_kernel, heads),
        [((8 + half, VDIM), F32)],
        (mix_lambda, met, query_new, key_new, value_new, head_gain.reshape(1, VDIM)),
        "sa",
    )
    (parts,) = call(
        functools.partial(local_kernel, peers, heads), [((peers * (2 * half + 1), VDIM), F32)], (prompt, w, query_new)
    )
    parts = parts.reshape(peers, 1, (2 * half + 1) * VDIM)
    parts = spread(parts, "sp").reshape(peers * (2 * half + 1), VDIM)
    (first_read,) = call(functools.partial(finish_kernel, peers, heads), [((count, cols), BF16)], (parts, fresh))

    found = [mine]
    for d in range(1, slices // 2):
        found.append(moved(mine, "tp", lambda i: i + 2 * d))
    for n in range(slices // 2):
        found.append(moved(found[n], "tp", lambda i: i ^ 1))
    key_cache, value_cache = call(
        functools.partial(block_kernel, slices),
        [((peers * sub, cols), BF16)] * 2,
        (*found, w),
        "a" * (slices + 1),
        [
            pltpu.VMEM((slices, peers * sub, depth), BF16),
            pltpu.VMEM((slices, depth, 2 * cols), BF16),
            pltpu.SemaphoreType.DMA((slices, 2)),
        ],
        LIMIT,
    )
    shape = (1, peers, sub, cols)
    return key_cache.reshape(shape), value_cache.reshape(shape), first_read


def solution(mesh):
    return jax.shard_map(
        inner,
        mesh=mesh,
        in_specs=(
            P("grp", "sp", None),
            P("sp", "tp"),
            P("sp", "tp"),
            P("grp", "tp"),
            P("grp", "tp"),
            P("grp", "tp"),
            P("tp"),
            P(),
        ),
        out_specs=(
            P(("grp", "sp"), None, None, "tp"),
            P(("grp", "sp"), None, None, "tp"),
            P("grp", "tp"),
        ),
        check_vma=False,
    )
```

```python
import functools
import jax
import jax.numpy as jnp
from jax import lax
from jax.experimental import pallas as pl
from jax.experimental.pallas import tpu as pltpu
from jax.sharding import PartitionSpec as P

HALF = 64
VDIM = 128
W_SHIFT = 2.0**18
F32 = jnp.float32
BF16 = jnp.bfloat16
NEG = -1e30
LIMIT = 16


def row_dot(a, b, precision=None):
    return lax.dot_general(a, b, (((1,), (1,)), ((), ())), preferred_element_type=F32, precision=precision)


def select_rows(rows, query, count, heads, pairs):
    width = query.shape[1]
    r = lax.broadcasted_iota(jnp.int32, (rows, width), 0)
    lane = lax.broadcasted_iota(jnp.int32, (rows, width), 1)
    out = jnp.zeros((rows, width), F32)
    for b in range(count):
        q = jnp.broadcast_to(query[b : b + 1, :].astype(F32), (rows, width))
        out = jnp.where((r // heads) % count == b, q, out)
    slot = (r % heads) * pairs + r // (count * heads)
    return jnp.where(lane // HALF == slot, out, 0.0)


def local_kernel(heads, x_ref, w_ref, q_ref, pay_ref):
    count, piece, width = x_ref.shape
    rows = 2 * count * heads
    cols = heads * 2 * HALF
    x = x_ref[...].reshape(count * piece, width)
    keys = jnp.dot(x, w_ref[:, :cols], preferred_element_type=F32).astype(BF16)
    values = jnp.dot(x, w_ref[:, cols:], preferred_element_type=F32).astype(BF16)
    picked = select_rows(rows, q_ref[...], count, heads, 2)
    scores = row_dot(picked.astype(BF16), keys) * HALF**-0.5
    r = lax.broadcasted_iota(jnp.int32, scores.shape, 0)
    at = lax.broadcasted_iota(jnp.int32, scores.shape, 1)
    scores = jnp.where((r // heads) % count == at // piece, scores, NEG)
    top = jnp.max(scores, axis=1, keepdims=True)
    weights = jnp.exp(scores - top)
    total = jnp.sum(weights, axis=1, keepdims=True)
    full = 0.0
    for p in three(weights):
        full += jnp.dot(p, values, preferred_element_type=F32)
    r = lax.broadcasted_iota(jnp.int32, (rows, VDIM), 0)
    part = jnp.zeros((rows, VDIM), F32)
    for h in range(heads):
        part = jnp.where(r % heads == h, full[:, h * VDIM : (h + 1) * VDIM], part)
    part = part / total
    power = jnp.ceil(jnp.log2(jnp.maximum(jnp.max(jnp.abs(part), axis=1, keepdims=True), 1e-30)))
    pay_ref[:rows, :] = part * jnp.exp2(-power)
    pay_ref[rows:, :] = jnp.zeros((pay_ref.shape[0] - rows, VDIM), F32)
    pieces = [p.astype(F32) * 256.0**n for x in (top / 64, total) for n, p in enumerate(three(x))]
    pay_ref[rows : rows + 1, :] = as_line([*pieces, power])


def three(x):
    high = x.astype(BF16)
    rest = x - high.astype(F32)
    middle = rest.astype(BF16)
    return high, middle, (rest - middle.astype(F32)).astype(BF16)


def as_line(columns):
    rows = sum(c.shape[0] for c in columns)
    both = jnp.concatenate([*columns, jnp.zeros((VDIM - rows, 1), F32)], axis=0)
    return jnp.broadcast_to(both, (VDIM, VDIM)).T[:1]


def fresh_kernel(heads, lam_ref, q_ref, kn_ref, vn_ref, gain_ref, out_ref):
    count = vn_ref.shape[0]
    half = count * heads
    rows = 2 * half
    fresh = select_rows(rows, q_ref[...], count, heads, 2) * select_rows(rows, kn_ref[...], count, heads, 2)
    out_ref[0:1, :] = as_line([jnp.sum(fresh, axis=1, keepdims=True) * HALF**-0.5])
    lane = lax.broadcasted_iota(jnp.int32, (1, VDIM), 1)
    sign = jnp.ones((1, VDIM), F32)
    for h in range(heads):
        sign = jnp.where((lane >= half) & (lane % heads == h), -lam_ref[h], sign)
    out_ref[1:2, :] = sign
    out_ref[2:3, :] = gain_ref[...]
    out_ref[3:8, :] = jnp.zeros((5, VDIM), F32)
    values = vn_ref[...].astype(F32)
    for b in range(count):
        for h in range(heads):
            n = 8 + b * heads + h
            out_ref[n : n + 1, :] = values[b : b + 1, h * VDIM : (h + 1) * VDIM]


def row_of_each(part_ref, r):
    each = part_ref.shape[2] // VDIM
    return part_ref[r // each, :, (r % each) * VDIM : (r % each + 1) * VDIM]


def finish_kernel(heads, part_ref, new_ref, out_ref):
    count = out_ref.shape[0]
    half = count * heads
    rows = 2 * half
    fresh = new_ref[0:1, :]
    stats = row_of_each(part_ref, rows)
    piece = [pltpu.roll(stats, (VDIM - n * rows) % VDIM, 1) for n in range(7)]
    tops = (piece[0] + piece[1] / 256.0 + piece[2] / 65536.0) * 64
    totals = piece[3] + piece[4] / 256.0 + piece[5] / 65536.0
    power = piece[6]
    top = jnp.maximum(jnp.max(tops, axis=0, keepdims=True), fresh)
    scale = jnp.exp(jnp.minimum(tops - top, 0.0))
    own = jnp.exp(fresh - top)
    total = jnp.sum(totals * scale, axis=0, keepdims=True) + own
    scale = scale * totals * jnp.exp2(power) * (new_ref[1:2, :] / total)
    own = own * (new_ref[1:2, :] / total)
    mine = (own + pltpu.roll(own, VDIM - half, 1)).astype(BF16).astype(F32)
    for b in range(count):
        for h in range(heads):
            n = b * heads + h
            reads = 0.0
            for r in (n, n + half):
                reads += scale[:, r : r + 1] * row_of_each(part_ref, r)
            reads = jnp.sum(reads, axis=0, keepdims=True)
            reads += mine[:, n : n + 1] * new_ref[8 + n : 9 + n, :]
            mean = jnp.mean(reads * reads, axis=1, keepdims=True)
            normed = reads * lax.rsqrt(mean + 1e-06) * new_ref[2:3, :]
            out_ref[b : b + 1, h * VDIM : (h + 1) * VDIM] = normed.astype(BF16)


def block_kernel(slices, *refs):
    x_refs, (w_ref, k_ref, v_ref, x_buf, w_buf, sem) = refs[:slices], refs[slices:]
    rows, depth = x_refs[0].shape
    cols = k_ref.shape[1]
    t = lax.axis_index("tp")
    who = [lax.rem(t + slices - 2 * d, slices) for d in range(slices // 2)]
    who += [lax.bitwise_xor(n, 1) for n in who]
    moves = []
    for n in range(slices):
        w = pl.ds(pl.multiple_of(who[n] * depth, depth), depth)
        moves.append(
            [
                pltpu.make_async_copy(w_ref.at[w, :], w_buf.at[n], sem.at[n, 0]),
                pltpu.make_async_copy(x_refs[n], x_buf.at[n], sem.at[n, 1]),
            ]
        )
        for m in moves[n]:
            m.start()
    step = rows // 4
    for at in range(0, rows, step):
        acc = 0.0
        for n in range(slices):
            if at == 0:
                for m in moves[n]:
                    m.wait()
            acc += jnp.dot(x_buf[n, at : at + step, :], w_buf[n], preferred_element_type=F32)
        k_ref[at : at + step, :] = acc[:, :cols].astype(BF16)
        v_ref[at : at + step, :] = acc[:, cols:].astype(BF16)


def call(kernel, outs, args, spaces="", scratch=(), limit=16):
    kinds = {"s": pltpu.SMEM, "a": pl.ANY, "v": pltpu.VMEM}
    spaces = spaces.ljust(len(args), "v")
    return pl.pallas_call(
        kernel,
        out_shape=[jax.ShapeDtypeStruct(s, d) for s, d in outs],
        in_specs=[pl.BlockSpec(memory_space=kinds[c]) for c in spaces],
        out_specs=[pl.BlockSpec(memory_space=pltpu.VMEM)] * len(outs),
        scratch_shapes=scratch,
        compiler_params=pltpu.CompilerParams(vmem_limit_bytes=int(limit * 2**20)),
    )(*args)


def spread(x, axis):
    return lax.all_to_all(x, axis, 0, 0, tiled=True)


def moved(x, axis, step):
    n = lax.axis_size(axis)
    return lax.ppermute(x, axis, [(i, step(i) % n) for i in range(n)])


def inner(prompt, w_key, w_value, query_new, key_new, value_new, mix_lambda, head_gain):
    count, piece, width = prompt.shape
    peers = lax.axis_size("sp")
    slices = lax.axis_size("tp")
    groups = peers // count
    sub = piece // groups
    heads = mix_lambda.shape[0]
    cols = w_key.shape[1]
    half = count * heads
    t = lax.axis_index("tp")

    depth = width // slices
    mine = lax.dynamic_slice_in_dim(prompt, t * depth, depth, 2).reshape(peers, sub, depth)
    w = jnp.concatenate([w_key, w_value], axis=1)
    w = (w.astype(F32) * W_SHIFT).astype(jnp.float16)
    mine, w = lax.optimization_barrier((mine, w))
    w = lax.all_gather(w, "sp", axis=0, tiled=True)
    w = (w.astype(F32) * (1 / W_SHIFT)).astype(BF16)
    w, mine = lax.optimization_barrier((w, mine))
    mine = spread(mine, "sp").reshape(peers * sub, depth)

    (fresh,) = call(
        functools.partial(fresh_kernel, heads),
        [((8 + half, VDIM), F32)],
        (mix_lambda, query_new, key_new, value_new, head_gain.reshape(1, VDIM)),
        "s",
    )
    each = half + 1
    (pay,) = call(functools.partial(local_kernel, heads), [((2 * each, VDIM), F32)], (prompt, w, query_new))
    parts = jnp.broadcast_to(pay.reshape(2, each * VDIM).astype(jnp.float16), (peers, 2, each * VDIM))
    parts = spread(parts, "sp")
    parts = parts.astype(F32).transpose(1, 0, 2)
    (first_read,) = call(functools.partial(finish_kernel, heads), [((count, cols), BF16)], (parts, fresh))

    found = [mine]
    for d in range(1, slices // 2):
        found.append(moved(mine, "tp", lambda i: i + 2 * d))
    for n in range(slices // 2):
        found.append(moved(found[n], "tp", lambda i: i ^ 1))
    key_cache, value_cache = call(
        functools.partial(block_kernel, slices),
        [((peers * sub, cols), BF16)] * 2,
        (*found, w),
        "a" * (slices + 1),
        [
            pltpu.VMEM((slices, peers * sub, depth), BF16),
            pltpu.VMEM((slices, depth, 2 * cols), BF16),
            pltpu.SemaphoreType.DMA((slices, 2)),
        ],
        LIMIT,
    )
    shape = (1, peers, sub, cols)
    return key_cache.reshape(shape), value_cache.reshape(shape), first_read


def solution(mesh):
    return jax.shard_map(
        inner,
        mesh=mesh,
        in_specs=(
            P("grp", "sp", None),
            P("sp", "tp"),
            P("sp", "tp"),
            P("grp", "tp"),
            P("grp", "tp"),
            P("grp", "tp"),
            P("tp"),
            P(),
        ),
        out_specs=(
            P(("grp", "sp"), None, None, "tp"),
            P(("grp", "sp"), None, None, "tp"),
            P("grp", "tp"),
        ),
        check_vma=False,
    )
```

```python
import functools
import jax
import jax.numpy as jnp
from jax import lax
from jax.experimental import pallas as pl
from jax.experimental.pallas import tpu as pltpu
from jax.sharding import PartitionSpec as P

HALF = 64
VDIM = 128
W_SHIFT = 2.0**18
F32 = jnp.float32
BF16 = jnp.bfloat16
NEG = -1e30


def row_dot(a, b, precision=None):
    return lax.dot_general(a, b, (((1,), (1,)), ((), ())), preferred_element_type=F32, precision=precision)


def select_rows(rows, query, count, heads, pairs):
    width = query.shape[1]
    r = lax.broadcasted_iota(jnp.int32, (rows, width), 0)
    lane = lax.broadcasted_iota(jnp.int32, (rows, width), 1)
    out = jnp.zeros((rows, width), F32)
    for b in range(count):
        q = jnp.broadcast_to(query[b : b + 1, :].astype(F32), (rows, width))
        out = jnp.where((r // heads) % count == b, q, out)
    slot = (r % heads) * pairs + r // (count * heads)
    return jnp.where(lane // HALF == slot, out, 0.0)


def local_kernel(heads, x_ref, w_ref, q_ref, pay_ref):
    count, piece, width = x_ref.shape
    rows = 2 * count * heads
    cols = heads * 2 * HALF
    x = x_ref[...].reshape(count * piece, width)
    keys = jnp.dot(x, w_ref[:, :cols], preferred_element_type=F32).astype(BF16)
    values = jnp.dot(x, w_ref[:, cols:], preferred_element_type=F32).astype(BF16)
    picked = select_rows(rows, q_ref[...], count, heads, 2)
    scores = row_dot(picked.astype(BF16), keys) * HALF**-0.5
    r = lax.broadcasted_iota(jnp.int32, scores.shape, 0)
    at = lax.broadcasted_iota(jnp.int32, scores.shape, 1)
    scores = jnp.where((r // heads) % count == at // piece, scores, NEG)
    top = jnp.max(scores, axis=1, keepdims=True)
    weights = jnp.exp(scores - top)
    total = jnp.sum(weights, axis=1, keepdims=True)
    full = 0.0
    for p in three(weights):
        full += jnp.dot(p, values, preferred_element_type=F32)
    r = lax.broadcasted_iota(jnp.int32, (rows, VDIM), 0)
    part = jnp.zeros((rows, VDIM), F32)
    for h in range(heads):
        part = jnp.where(r % heads == h, full[:, h * VDIM : (h + 1) * VDIM], part)
    part = part / total
    power = jnp.ceil(jnp.log2(jnp.maximum(jnp.max(jnp.abs(part), axis=1, keepdims=True), 1e-30)))
    pay_ref[:rows, :] = part * jnp.exp2(-power)
    pay_ref[rows:, :] = jnp.zeros((pay_ref.shape[0] - rows, VDIM), F32)
    pieces = [p.astype(F32) * 256.0**n for x in (top / 64, total) for n, p in enumerate(three(x))]
    pay_ref[rows : rows + 1, :] = as_line([*pieces, power])


def three(x):
    high = x.astype(BF16)
    rest = x - high.astype(F32)
    middle = rest.astype(BF16)
    return high, middle, (rest - middle.astype(F32)).astype(BF16)


def as_line(columns):
    rows = sum(c.shape[0] for c in columns)
    both = jnp.concatenate([*columns, jnp.zeros((VDIM - rows, 1), F32)], axis=0)
    return jnp.broadcast_to(both, (VDIM, VDIM)).T[:1]


def fresh_kernel(heads, lam_ref, q_ref, kn_ref, vn_ref, gain_ref, out_ref):
    count = vn_ref.shape[0]
    half = count * heads
    rows = 2 * half
    fresh = select_rows(rows, q_ref[...], count, heads, 2) * select_rows(rows, kn_ref[...], count, heads, 2)
    out_ref[0:1, :] = as_line([jnp.sum(fresh, axis=1, keepdims=True) * HALF**-0.5])
    lane = lax.broadcasted_iota(jnp.int32, (1, VDIM), 1)
    sign = jnp.ones((1, VDIM), F32)
    for h in range(heads):
        sign = jnp.where((lane >= half) & (lane % heads == h), -lam_ref[h], sign)
    out_ref[1:2, :] = sign
    out_ref[2:3, :] = gain_ref[...]
    out_ref[3:8, :] = jnp.zeros((5, VDIM), F32)
    values = vn_ref[...].astype(F32)
    for b in range(count):
        for h in range(heads):
            n = 8 + b * heads + h
            out_ref[n : n + 1, :] = values[b : b + 1, h * VDIM : (h + 1) * VDIM]


def row_of_each(part_ref, r):
    each = part_ref.shape[2] // VDIM
    return part_ref[r // each, :, (r % each) * VDIM : (r % each + 1) * VDIM]


def finish_kernel(heads, part_ref, new_ref, out_ref):
    count = out_ref.shape[0]
    half = count * heads
    rows = 2 * half
    fresh = new_ref[0:1, :]
    stats = row_of_each(part_ref, rows)
    piece = [pltpu.roll(stats, (VDIM - n * rows) % VDIM, 1) for n in range(7)]
    tops = (piece[0] + piece[1] / 256.0 + piece[2] / 65536.0) * 64
    totals = piece[3] + piece[4] / 256.0 + piece[5] / 65536.0
    power = piece[6]
    top = jnp.maximum(jnp.max(tops, axis=0, keepdims=True), fresh)
    scale = jnp.exp(jnp.minimum(tops - top, 0.0))
    own = jnp.exp(fresh - top)
    total = jnp.sum(totals * scale, axis=0, keepdims=True) + own
    scale = scale * totals * jnp.exp2(power) * (new_ref[1:2, :] / total)
    own = own * (new_ref[1:2, :] / total)
    mine = (own + pltpu.roll(own, VDIM - half, 1)).astype(BF16).astype(F32)
    for b in range(count):
        for h in range(heads):
            n = b * heads + h
            reads = 0.0
            for r in (n, n + half):
                reads += scale[:, r : r + 1] * row_of_each(part_ref, r)
            reads = jnp.sum(reads, axis=0, keepdims=True)
            reads += mine[:, n : n + 1] * new_ref[8 + n : 9 + n, :]
            mean = jnp.mean(reads * reads, axis=1, keepdims=True)
            normed = reads * lax.rsqrt(mean + 1e-06) * new_ref[2:3, :]
            out_ref[b : b + 1, h * VDIM : (h + 1) * VDIM] = normed.astype(BF16)


def slices_kernel(chips, x_refs, w_ref, where, acc_ref, x_buf, w_buf, sem):
    rows = x_refs[0].shape[0]
    moves = []
    for n in range(chips):
        moves.append(
            [
                pltpu.make_async_copy(w_ref.at[where(n)], w_buf.at[n], sem.at[n, 0]),
                pltpu.make_async_copy(x_refs[n], x_buf.at[n], sem.at[n, 1]),
            ]
        )
        for m in moves[n]:
            m.start()
    step = rows // 4
    for at in range(0, rows, step):
        acc = 0.0
        for n in range(chips):
            if at == 0:
                for m in moves[n]:
                    m.wait()
            acc += jnp.dot(x_buf[n, at : at + step, :], w_buf[n], preferred_element_type=F32)
        acc_ref[at : at + step, :] = acc


def theirs_kernel(chips, *refs):
    t = lax.axis_index("tp")
    where = lambda n: lax.div(lax.rem(t + 2 * chips - 2 * n, 2 * chips), 2)
    slices_kernel(chips, refs[:chips], refs[chips], where, *refs[chips + 1 :])


def ours_kernel(chips, *refs):
    t = lax.axis_index("tp")
    where = lambda n: lax.rem(t + 2 * chips - 2 * n, 2 * chips)
    slices_kernel(chips, refs[:chips], refs[chips], where, *refs[chips + 1 :])


def join_kernel(ours_ref, swapped_ref, k_ref, v_ref):
    cols = k_ref.shape[1]
    k_ref[...] = (ours_ref[:, :cols] + swapped_ref[:, :cols]).astype(BF16)
    v_ref[...] = (ours_ref[:, cols:] + swapped_ref[:, cols:]).astype(BF16)


def call(kernel, outs, args, spaces="", scratch=(), limit=16):
    kinds = {"s": pltpu.SMEM, "a": pl.ANY, "v": pltpu.VMEM}
    spaces = spaces.ljust(len(args), "v")
    return pl.pallas_call(
        kernel,
        out_shape=[jax.ShapeDtypeStruct(s, d) for s, d in outs],
        in_specs=[pl.BlockSpec(memory_space=kinds[c]) for c in spaces],
        out_specs=[pl.BlockSpec(memory_space=pltpu.VMEM)] * len(outs),
        scratch_shapes=scratch,
        compiler_params=pltpu.CompilerParams(vmem_limit_bytes=int(limit * 2**20)),
    )(*args)


def spread(x, axis):
    return lax.all_to_all(x, axis, 0, 0, tiled=True)


def moved(x, axis, step):
    n = lax.axis_size(axis)
    return lax.ppermute(x, axis, [(i, step(i) % n) for i in range(n)])


def inner(prompt, w_key, w_value, query_new, key_new, value_new, mix_lambda, head_gain):
    count, piece, width = prompt.shape
    peers = lax.axis_size("sp")
    slices = lax.axis_size("tp")
    groups = peers // count
    sub = piece // groups
    heads = mix_lambda.shape[0]
    cols = w_key.shape[1]
    half = count * heads
    t = lax.axis_index("tp")

    depth = width // slices
    mine = lax.dynamic_slice_in_dim(prompt, t * depth, depth, 2).reshape(peers, sub, depth)
    w = jnp.concatenate([w_key, w_value], axis=1)
    w = (w.astype(F32) * W_SHIFT).astype(jnp.float16)
    mine, w = lax.optimization_barrier((mine, w))
    w = lax.all_gather(w, "sp", axis=0, tiled=True)
    w = (w.astype(F32) * (1 / W_SHIFT)).astype(BF16)

    (fresh,) = call(
        functools.partial(fresh_kernel, heads),
        [((8 + half, VDIM), F32)],
        (mix_lambda, query_new, key_new, value_new, head_gain.reshape(1, VDIM)),
        "s",
    )
    each = half + 1
    (pay,) = call(functools.partial(local_kernel, heads), [((2 * each, VDIM), F32)], (prompt, w, query_new))
    pay, mine = lax.optimization_barrier((pay, mine))
    mine = spread(mine, "sp").reshape(peers * sub, depth)
    parts = jnp.broadcast_to(pay.reshape(2, each * VDIM).astype(jnp.float16), (peers, 2, each * VDIM))
    parts = spread(parts, "sp")
    parts = parts.astype(F32).transpose(1, 0, 2)
    (first_read,) = call(functools.partial(finish_kernel, heads), [((count, cols), BF16)], (parts, fresh))

    chips = slices // 2
    w = w.reshape(slices, depth, 2 * cols)
    lent = lax.dynamic_index_in_dim(w.reshape(chips, 2, depth, 2 * cols), 1 - t % 2, 1, False)
    lent = moved(lent, "tp", lambda i: i ^ 1)
    found = [mine]
    for d in range(1, chips):
        found.append(moved(mine, "tp", lambda i: i + 2 * d))
    scratch = [
        pltpu.VMEM((chips, peers * sub, depth), BF16),
        pltpu.VMEM((chips, depth, 2 * cols), BF16),
        pltpu.SemaphoreType.DMA((chips, 2)),
    ]
    partial = [((peers * sub, 2 * cols), F32)]
    anywhere = "a" * (chips + 1)
    (theirs,) = call(functools.partial(theirs_kernel, chips), partial, (*found, lent), anywhere, scratch)
    theirs = moved(theirs, "tp", lambda i: i ^ 1)
    (ours,) = call(functools.partial(ours_kernel, chips), partial, (*found, w), anywhere, scratch)
    key_cache, value_cache = call(join_kernel, [((peers * sub, cols), BF16)] * 2, (ours, theirs))
    shape = (1, peers, sub, cols)
    return key_cache.reshape(shape), value_cache.reshape(shape), first_read


def solution(mesh):
    return jax.shard_map(
        inner,
        mesh=mesh,
        in_specs=(
            P("grp", "sp", None),
            P("sp", "tp"),
            P("sp", "tp"),
            P("grp", "tp"),
            P("grp", "tp"),
            P("grp", "tp"),
            P("tp"),
            P(),
        ),
        out_specs=(
            P(("grp", "sp"), None, None, "tp"),
            P(("grp", "sp"), None, None, "tp"),
            P("grp", "tp"),
        ),
        check_vma=False,
    )
```

```python
import functools
import jax
import jax.numpy as jnp
from jax import lax
from jax.experimental import pallas as pl
from jax.experimental.pallas import tpu as pltpu
from jax.sharding import PartitionSpec as P

HALF = 64
VDIM = 128
W_SHIFT = 2.0**18
F32 = jnp.float32
BF16 = jnp.bfloat16
NEG = -1e30


def row_dot(a, b, precision=None):
    return lax.dot_general(a, b, (((1,), (1,)), ((), ())), preferred_element_type=F32, precision=precision)


def select_rows(rows, query, count, heads, pairs):
    width = query.shape[1]
    r = lax.broadcasted_iota(jnp.int32, (rows, width), 0)
    lane = lax.broadcasted_iota(jnp.int32, (rows, width), 1)
    out = jnp.zeros((rows, width), F32)
    for b in range(count):
        q = jnp.broadcast_to(query[b : b + 1, :].astype(F32), (rows, width))
        out = jnp.where((r // heads) % count == b, q, out)
    slot = (r % heads) * pairs + r // (count * heads)
    return jnp.where(lane // HALF == slot, out, 0.0)


def local_kernel(heads, x_ref, blocks_ref, w_ref, q_ref, pay_ref, mine_ref, sem):
    depth = mine_ref.shape[2]
    lanes = pl.ds(pl.multiple_of(lax.axis_index("tp") * depth, depth), depth)
    cut = pltpu.make_async_copy(blocks_ref.at[:, :, lanes], mine_ref, sem)
    cut.start()
    count, piece, width = x_ref.shape
    rows = 2 * count * heads
    cols = heads * 2 * HALF
    x = x_ref[...].reshape(count * piece, width)
    keys = jnp.dot(x, w_ref[:, :cols], preferred_element_type=F32).astype(BF16)
    values = jnp.dot(x, w_ref[:, cols:], preferred_element_type=F32).astype(BF16)
    picked = select_rows(rows, q_ref[...], count, heads, 2)
    scores = row_dot(picked.astype(BF16), keys) * HALF**-0.5
    r = lax.broadcasted_iota(jnp.int32, scores.shape, 0)
    at = lax.broadcasted_iota(jnp.int32, scores.shape, 1)
    scores = jnp.where((r // heads) % count == at // piece, scores, NEG)
    top = jnp.max(scores, axis=1, keepdims=True)
    weights = jnp.exp(scores - top)
    total = jnp.sum(weights, axis=1, keepdims=True)
    full = 0.0
    for p in three(weights):
        full += jnp.dot(p, values, preferred_element_type=F32)
    r = lax.broadcasted_iota(jnp.int32, (rows, VDIM), 0)
    part = jnp.zeros((rows, VDIM), F32)
    for h in range(heads):
        part = jnp.where(r % heads == h, full[:, h * VDIM : (h + 1) * VDIM], part)
    part = part / total
    power = jnp.ceil(jnp.log2(jnp.maximum(jnp.max(jnp.abs(part), axis=1, keepdims=True), 1e-30)))
    pay_ref[:rows, :] = part * jnp.exp2(-power)
    pay_ref[rows:, :] = jnp.zeros((pay_ref.shape[0] - rows, VDIM), F32)
    pieces = [p.astype(F32) * 256.0**n for x in (top / 64, total) for n, p in enumerate(three(x))]
    pay_ref[rows : rows + 1, :] = as_line([*pieces, power])
    cut.wait()


def three(x):
    high = x.astype(BF16)
    rest = x - high.astype(F32)
    middle = rest.astype(BF16)
    return high, middle, (rest - middle.astype(F32)).astype(BF16)


def as_line(columns):
    rows = sum(c.shape[0] for c in columns)
    both = jnp.concatenate([*columns, jnp.zeros((VDIM - rows, 1), F32)], axis=0)
    return jnp.broadcast_to(both, (VDIM, VDIM)).T[:1]


def fresh_kernel(heads, lam_ref, q_ref, kn_ref, vn_ref, gain_ref, out_ref):
    count = vn_ref.shape[0]
    half = count * heads
    rows = 2 * half
    fresh = select_rows(rows, q_ref[...], count, heads, 2) * select_rows(rows, kn_ref[...], count, heads, 2)
    out_ref[0:1, :] = as_line([jnp.sum(fresh, axis=1, keepdims=True) * HALF**-0.5])
    lane = lax.broadcasted_iota(jnp.int32, (1, VDIM), 1)
    sign = jnp.ones((1, VDIM), F32)
    for h in range(heads):
        sign = jnp.where((lane >= half) & (lane % heads == h), -lam_ref[h], sign)
    out_ref[1:2, :] = sign
    out_ref[2:3, :] = gain_ref[...]
    out_ref[3:8, :] = jnp.zeros((5, VDIM), F32)
    values = vn_ref[...].astype(F32)
    for b in range(count):
        for h in range(heads):
            n = 8 + b * heads + h
            out_ref[n : n + 1, :] = values[b : b + 1, h * VDIM : (h + 1) * VDIM]


def row_of_each(part_ref, r):
    each = part_ref.shape[2] // VDIM
    return part_ref[r // each, :, (r % each) * VDIM : (r % each + 1) * VDIM]


def finish_kernel(heads, part_ref, new_ref, out_ref):
    count = out_ref.shape[0]
    half = count * heads
    rows = 2 * half
    fresh = new_ref[0:1, :]
    stats = row_of_each(part_ref, rows)
    piece = [pltpu.roll(stats, (VDIM - n * rows) % VDIM, 1) for n in range(7)]
    tops = (piece[0] + piece[1] / 256.0 + piece[2] / 65536.0) * 64
    totals = piece[3] + piece[4] / 256.0 + piece[5] / 65536.0
    power = piece[6]
    top = jnp.maximum(jnp.max(tops, axis=0, keepdims=True), fresh)
    scale = jnp.exp(jnp.minimum(tops - top, 0.0))
    own = jnp.exp(fresh - top)
    total = jnp.sum(totals * scale, axis=0, keepdims=True) + own
    scale = scale * totals * jnp.exp2(power) * (new_ref[1:2, :] / total)
    own = own * (new_ref[1:2, :] / total)
    mine = (own + pltpu.roll(own, VDIM - half, 1)).astype(BF16).astype(F32)
    for b in range(count):
        for h in range(heads):
            n = b * heads + h
            reads = 0.0
            for r in (n, n + half):
                reads += scale[:, r : r + 1] * row_of_each(part_ref, r)
            reads = jnp.sum(reads, axis=0, keepdims=True)
            reads += mine[:, n : n + 1] * new_ref[8 + n : 9 + n, :]
            mean = jnp.mean(reads * reads, axis=1, keepdims=True)
            normed = reads * lax.rsqrt(mean + 1e-06) * new_ref[2:3, :]
            out_ref[b : b + 1, h * VDIM : (h + 1) * VDIM] = normed.astype(BF16)


def slices_kernel(chips, x_refs, w_ref, where, acc_ref, x_buf, w_buf, sem):
    rows = x_refs[0].shape[0]
    moves = []
    for n in range(chips):
        moves.append(
            [
                pltpu.make_async_copy(w_ref.at[where(n)], w_buf.at[n], sem.at[n, 0]),
                pltpu.make_async_copy(x_refs[n], x_buf.at[n], sem.at[n, 1]),
            ]
        )
        for m in moves[n]:
            m.start()
    step = rows // 4
    for at in range(0, rows, step):
        acc = 0.0
        for n in range(chips):
            if at == 0:
                for m in moves[n]:
                    m.wait()
            acc += jnp.dot(x_buf[n, at : at + step, :], w_buf[n], preferred_element_type=F32)
        acc_ref[at : at + step, :] = acc


def theirs_kernel(chips, *refs):
    t = lax.axis_index("tp")
    where = lambda n: lax.div(lax.rem(t + 2 * chips - 2 * n, 2 * chips), 2)
    slices_kernel(chips, refs[:chips], refs[chips], where, *refs[chips + 1 :])


def ours_kernel(chips, *refs):
    t = lax.axis_index("tp")
    where = lambda n: lax.rem(t + 2 * chips - 2 * n, 2 * chips)
    slices_kernel(chips, refs[:chips], refs[chips], where, *refs[chips + 1 :])


def join_kernel(ours_ref, swapped_ref, k_ref, v_ref):
    cols = k_ref.shape[1]
    k_ref[...] = (ours_ref[:, :cols] + swapped_ref[:, :cols]).astype(BF16)
    v_ref[...] = (ours_ref[:, cols:] + swapped_ref[:, cols:]).astype(BF16)


def call(kernel, outs, args, spaces="", scratch=(), limit=16):
    kinds = {"s": pltpu.SMEM, "a": pl.ANY, "v": pltpu.VMEM}
    spaces = spaces.ljust(len(args), "v")
    return pl.pallas_call(
        kernel,
        out_shape=[jax.ShapeDtypeStruct(s, d) for s, d in outs],
        in_specs=[pl.BlockSpec(memory_space=kinds[c]) for c in spaces],
        out_specs=[pl.BlockSpec(memory_space=pltpu.VMEM)] * len(outs),
        scratch_shapes=scratch,
        compiler_params=pltpu.CompilerParams(vmem_limit_bytes=int(limit * 2**20)),
    )(*args)


def spread(x, axis):
    return lax.all_to_all(x, axis, 0, 0, tiled=True)


def moved(x, axis, step):
    n = lax.axis_size(axis)
    return lax.ppermute(x, axis, [(i, step(i) % n) for i in range(n)])


def inner(prompt, w_key, w_value, query_new, key_new, value_new, mix_lambda, head_gain):
    count, piece, width = prompt.shape
    peers = lax.axis_size("sp")
    slices = lax.axis_size("tp")
    groups = peers // count
    sub = piece // groups
    heads = mix_lambda.shape[0]
    cols = w_key.shape[1]
    half = count * heads
    t = lax.axis_index("tp")

    depth = width // slices
    w = jnp.concatenate([w_key, w_value], axis=1)
    w = (w.astype(F32) * W_SHIFT).astype(jnp.float16)
    w = lax.all_gather(w, "sp", axis=0, tiled=True)
    w = (w.astype(F32) * (1 / W_SHIFT)).astype(BF16)

    (fresh,) = call(
        functools.partial(fresh_kernel, heads),
        [((8 + half, VDIM), F32)],
        (mix_lambda, query_new, key_new, value_new, head_gain.reshape(1, VDIM)),
        "s",
    )
    each = half + 1
    pay, mine = call(
        functools.partial(local_kernel, heads),
        [((2 * each, VDIM), F32), ((peers, sub, depth), BF16)],
        (prompt, prompt.reshape(peers, sub, width), w, query_new),
        "va",
        [pltpu.SemaphoreType.DMA],
    )
    mine = spread(mine, "sp").reshape(peers * sub, depth)
    parts = jnp.broadcast_to(pay.reshape(2, each * VDIM).astype(jnp.float16), (peers, 2, each * VDIM))
    parts = spread(parts, "sp")
    parts = parts.astype(F32).transpose(1, 0, 2)
    (first_read,) = call(functools.partial(finish_kernel, heads), [((count, cols), BF16)], (parts, fresh))

    chips = slices // 2
    w = w.reshape(slices, depth, 2 * cols)
    lent = lax.dynamic_index_in_dim(w.reshape(chips, 2, depth, 2 * cols), 1 - t % 2, 1, False)
    lent = moved(lent, "tp", lambda i: i ^ 1)
    found = [mine]
    for d in range(1, chips):
        found.append(moved(mine, "tp", lambda i: i + 2 * d))
    scratch = [
        pltpu.VMEM((chips, peers * sub, depth), BF16),
        pltpu.VMEM((chips, depth, 2 * cols), BF16),
        pltpu.SemaphoreType.DMA((chips, 2)),
    ]
    partial = [((peers * sub, 2 * cols), F32)]
    anywhere = "a" * (chips + 1)
    (theirs,) = call(functools.partial(theirs_kernel, chips), partial, (*found, lent), anywhere, scratch)
    theirs = moved(theirs, "tp", lambda i: i ^ 1)
    (ours,) = call(functools.partial(ours_kernel, chips), partial, (*found, w), anywhere, scratch)
    key_cache, value_cache = call(join_kernel, [((peers * sub, cols), BF16)] * 2, (ours, theirs))
    shape = (1, peers, sub, cols)
    return key_cache.reshape(shape), value_cache.reshape(shape), first_read


def solution(mesh):
    return jax.shard_map(
        inner,
        mesh=mesh,
        in_specs=(
            P("grp", "sp", None),
            P("sp", "tp"),
            P("sp", "tp"),
            P("grp", "tp"),
            P("grp", "tp"),
            P("grp", "tp"),
            P("tp"),
            P(),
        ),
        out_specs=(
            P(("grp", "sp"), None, None, "tp"),
            P(("grp", "sp"), None, None, "tp"),
            P("grp", "tp"),
        ),
        check_vma=False,
    )
```

```python
import functools
import jax
import jax.numpy as jnp
from jax import lax
from jax.experimental import pallas as pl
from jax.experimental.pallas import tpu as pltpu
from jax.sharding import PartitionSpec as P

HALF = 64
VDIM = 128
W_SHIFT = 2.0**18
F32 = jnp.float32
BF16 = jnp.bfloat16
NEG = -1e30


def row_dot(a, b, precision=None):
    return lax.dot_general(a, b, (((1,), (1,)), ((), ())), preferred_element_type=F32, precision=precision)


def select_rows(rows, query, count, heads, pairs):
    width = query.shape[1]
    r = lax.broadcasted_iota(jnp.int32, (rows, width), 0)
    lane = lax.broadcasted_iota(jnp.int32, (rows, width), 1)
    out = jnp.zeros((rows, width), F32)
    for b in range(count):
        q = jnp.broadcast_to(query[b : b + 1, :].astype(F32), (rows, width))
        out = jnp.where((r // heads) % count == b, q, out)
    slot = (r % heads) * pairs + r // (count * heads)
    return jnp.where(lane // HALF == slot, out, 0.0)


def project_kernel(x_ref, blocks_ref, w_ref, keys_ref, values_ref, mine_ref, sem):
    count, piece, width = x_ref.shape
    cols = keys_ref.shape[1]
    depth = mine_ref.shape[2]
    lanes = pl.ds(pl.multiple_of(lax.axis_index("tp") * depth, depth), depth)
    cut = pltpu.make_async_copy(blocks_ref.at[:, :, lanes], mine_ref, sem)
    cut.start()
    x = x_ref[...].reshape(count * piece, width)
    keys_ref[...] = jnp.dot(x, w_ref[:, :cols], preferred_element_type=F32).astype(BF16)
    values_ref[...] = jnp.dot(x, w_ref[:, cols:], preferred_element_type=F32).astype(BF16)
    cut.wait()


def local_kernel(heads, keys_ref, values_ref, q_ref, pay_ref):
    count = q_ref.shape[0]
    piece = keys_ref.shape[0] // count
    rows = 2 * count * heads
    keys, values = keys_ref[...], values_ref[...]
    picked = select_rows(rows, q_ref[...], count, heads, 2)
    scores = row_dot(picked.astype(BF16), keys) * HALF**-0.5
    r = lax.broadcasted_iota(jnp.int32, scores.shape, 0)
    at = lax.broadcasted_iota(jnp.int32, scores.shape, 1)
    scores = jnp.where((r // heads) % count == at // piece, scores, NEG)
    top = jnp.max(scores, axis=1, keepdims=True)
    weights = jnp.exp(scores - top)
    total = jnp.sum(weights, axis=1, keepdims=True)
    full = 0.0
    for p in three(weights):
        full += jnp.dot(p, values, preferred_element_type=F32)
    r = lax.broadcasted_iota(jnp.int32, (rows, VDIM), 0)
    part = jnp.zeros((rows, VDIM), F32)
    for h in range(heads):
        part = jnp.where(r % heads == h, full[:, h * VDIM : (h + 1) * VDIM], part)
    part = part / total
    power = jnp.ceil(jnp.log2(jnp.maximum(jnp.max(jnp.abs(part), axis=1, keepdims=True), 1e-30)))
    pay_ref[:rows, :] = part * jnp.exp2(-power)
    pay_ref[rows:, :] = jnp.zeros((pay_ref.shape[0] - rows, VDIM), F32)
    pieces = [p.astype(F32) * 256.0**n for x in (top / 64, total) for n, p in enumerate(three(x))]
    pay_ref[rows : rows + 1, :] = as_line([*pieces, power])


def three(x):
    high = x.astype(BF16)
    rest = x - high.astype(F32)
    middle = rest.astype(BF16)
    return high, middle, (rest - middle.astype(F32)).astype(BF16)


def as_line(columns):
    rows = sum(c.shape[0] for c in columns)
    both = jnp.concatenate([*columns, jnp.zeros((VDIM - rows, 1), F32)], axis=0)
    return jnp.broadcast_to(both, (VDIM, VDIM)).T[:1]


def fresh_kernel(heads, lam_ref, q_ref, kn_ref, vn_ref, gain_ref, out_ref):
    count = vn_ref.shape[0]
    half = count * heads
    rows = 2 * half
    fresh = select_rows(rows, q_ref[...], count, heads, 2) * select_rows(rows, kn_ref[...], count, heads, 2)
    out_ref[0:1, :] = as_line([jnp.sum(fresh, axis=1, keepdims=True) * HALF**-0.5])
    lane = lax.broadcasted_iota(jnp.int32, (1, VDIM), 1)
    sign = jnp.ones((1, VDIM), F32)
    for h in range(heads):
        sign = jnp.where((lane >= half) & (lane % heads == h), -lam_ref[h], sign)
    out_ref[1:2, :] = sign
    out_ref[2:3, :] = gain_ref[...]
    out_ref[3:8, :] = jnp.zeros((5, VDIM), F32)
    values = vn_ref[...].astype(F32)
    for b in range(count):
        for h in range(heads):
            n = 8 + b * heads + h
            out_ref[n : n + 1, :] = values[b : b + 1, h * VDIM : (h + 1) * VDIM]


def row_of_each(part_ref, r):
    each = part_ref.shape[2] // VDIM
    return part_ref[r // each, :, (r % each) * VDIM : (r % each + 1) * VDIM]


def finish_kernel(heads, part_ref, new_ref, out_ref):
    count = out_ref.shape[0]
    half = count * heads
    rows = 2 * half
    fresh = new_ref[0:1, :]
    stats = row_of_each(part_ref, rows)
    piece = [pltpu.roll(stats, (VDIM - n * rows) % VDIM, 1) for n in range(7)]
    tops = (piece[0] + piece[1] / 256.0 + piece[2] / 65536.0) * 64
    totals = piece[3] + piece[4] / 256.0 + piece[5] / 65536.0
    power = piece[6]
    top = jnp.maximum(jnp.max(tops, axis=0, keepdims=True), fresh)
    scale = jnp.exp(jnp.minimum(tops - top, 0.0))
    own = jnp.exp(fresh - top)
    total = jnp.sum(totals * scale, axis=0, keepdims=True) + own
    scale = scale * totals * jnp.exp2(power) * (new_ref[1:2, :] / total)
    own = own * (new_ref[1:2, :] / total)
    mine = (own + pltpu.roll(own, VDIM - half, 1)).astype(BF16).astype(F32)
    for b in range(count):
        for h in range(heads):
            n = b * heads + h
            reads = 0.0
            for r in (n, n + half):
                reads += scale[:, r : r + 1] * row_of_each(part_ref, r)
            reads = jnp.sum(reads, axis=0, keepdims=True)
            reads += mine[:, n : n + 1] * new_ref[8 + n : 9 + n, :]
            mean = jnp.mean(reads * reads, axis=1, keepdims=True)
            normed = reads * lax.rsqrt(mean + 1e-06) * new_ref[2:3, :]
            out_ref[b : b + 1, h * VDIM : (h + 1) * VDIM] = normed.astype(BF16)


def slices_kernel(chips, x_refs, w_ref, where, acc_ref, x_buf, w_buf, sem):
    rows = x_refs[0].shape[0]
    moves = []
    for n in range(chips):
        moves.append(
            [
                pltpu.make_async_copy(w_ref.at[where(n)], w_buf.at[n], sem.at[n, 0]),
                pltpu.make_async_copy(x_refs[n], x_buf.at[n], sem.at[n, 1]),
            ]
        )
        for m in moves[n]:
            m.start()
    step = rows // 4
    for at in range(0, rows, step):
        acc = 0.0
        for n in range(chips):
            if at == 0:
                for m in moves[n]:
                    m.wait()
            acc += jnp.dot(x_buf[n, at : at + step, :], w_buf[n], preferred_element_type=F32)
        acc_ref[at : at + step, :] = acc


def theirs_kernel(chips, *refs):
    t = lax.axis_index("tp")
    where = lambda n: lax.div(lax.rem(t + 2 * chips - 2 * n, 2 * chips), 2)
    slices_kernel(chips, refs[:chips], refs[chips], where, *refs[chips + 1 :])


def ours_kernel(chips, *refs):
    t = lax.axis_index("tp")
    where = lambda n: lax.rem(t + 2 * chips - 2 * n, 2 * chips)
    slices_kernel(chips, refs[:chips], refs[chips], where, *refs[chips + 1 :])


def join_kernel(ours_ref, swapped_ref, k_ref, v_ref):
    cols = k_ref.shape[1]
    k_ref[...] = (ours_ref[:, :cols] + swapped_ref[:, :cols]).astype(BF16)
    v_ref[...] = (ours_ref[:, cols:] + swapped_ref[:, cols:]).astype(BF16)


def call(kernel, outs, args, spaces="", scratch=(), limit=16):
    kinds = {"s": pltpu.SMEM, "a": pl.ANY, "v": pltpu.VMEM}
    spaces = spaces.ljust(len(args), "v")
    return pl.pallas_call(
        kernel,
        out_shape=[jax.ShapeDtypeStruct(s, d) for s, d in outs],
        in_specs=[pl.BlockSpec(memory_space=kinds[c]) for c in spaces],
        out_specs=[pl.BlockSpec(memory_space=pltpu.VMEM)] * len(outs),
        scratch_shapes=scratch,
        compiler_params=pltpu.CompilerParams(vmem_limit_bytes=int(limit * 2**20)),
    )(*args)


def spread(x, axis):
    return lax.all_to_all(x, axis, 0, 0, tiled=True)


def moved(x, axis, step):
    n = lax.axis_size(axis)
    return lax.ppermute(x, axis, [(i, step(i) % n) for i in range(n)])


def inner(prompt, w_key, w_value, query_new, key_new, value_new, mix_lambda, head_gain):
    count, piece, width = prompt.shape
    peers = lax.axis_size("sp")
    slices = lax.axis_size("tp")
    groups = peers // count
    sub = piece // groups
    heads = mix_lambda.shape[0]
    cols = w_key.shape[1]
    half = count * heads
    t = lax.axis_index("tp")

    depth = width // slices
    w = jnp.concatenate([w_key, w_value], axis=1)
    w = (w.astype(F32) * W_SHIFT).astype(jnp.float16)
    w = lax.all_gather(w, "sp", axis=0, tiled=True)
    w = (w.astype(F32) * (1 / W_SHIFT)).astype(BF16)

    (fresh,) = call(
        functools.partial(fresh_kernel, heads),
        [((8 + half, VDIM), F32)],
        (mix_lambda, query_new, key_new, value_new, head_gain.reshape(1, VDIM)),
        "s",
    )
    each = half + 1
    keys, values, mine = call(
        project_kernel,
        [((count * piece, cols), BF16)] * 2 + [((peers, sub, depth), BF16)],
        (prompt, prompt.reshape(peers, sub, width), w),
        "va",
        [pltpu.SemaphoreType.DMA],
    )
    mine = spread(mine, "sp").reshape(peers * sub, depth)
    (pay,) = call(functools.partial(local_kernel, heads), [((2 * each, VDIM), F32)], (keys, values, query_new))
    parts = jnp.broadcast_to(pay.reshape(2, each * VDIM).astype(jnp.float16), (peers, 2, each * VDIM))
    parts = spread(parts, "sp")
    parts = parts.astype(F32).transpose(1, 0, 2)
    (first_read,) = call(functools.partial(finish_kernel, heads), [((count, cols), BF16)], (parts, fresh))

    chips = slices // 2
    w = w.reshape(slices, depth, 2 * cols)
    lent = lax.dynamic_index_in_dim(w.reshape(chips, 2, depth, 2 * cols), 1 - t % 2, 1, False)
    lent = moved(lent, "tp", lambda i: i ^ 1)
    found = [mine]
    for d in range(1, chips):
        found.append(moved(mine, "tp", lambda i: i + 2 * d))
    scratch = [
        pltpu.VMEM((chips, peers * sub, depth), BF16),
        pltpu.VMEM((chips, depth, 2 * cols), BF16),
        pltpu.SemaphoreType.DMA((chips, 2)),
    ]
    partial = [((peers * sub, 2 * cols), F32)]
    anywhere = "a" * (chips + 1)
    (theirs,) = call(functools.partial(theirs_kernel, chips), partial, (*found, lent), anywhere, scratch)
    theirs = moved(theirs, "tp", lambda i: i ^ 1)
    (ours,) = call(functools.partial(ours_kernel, chips), partial, (*found, w), anywhere, scratch)
    key_cache, value_cache = call(join_kernel, [((peers * sub, cols), BF16)] * 2, (ours, theirs))
    shape = (1, peers, sub, cols)
    return key_cache.reshape(shape), value_cache.reshape(shape), first_read


def solution(mesh):
    return jax.shard_map(
        inner,
        mesh=mesh,
        in_specs=(
            P("grp", "sp", None),
            P("sp", "tp"),
            P("sp", "tp"),
            P("grp", "tp"),
            P("grp", "tp"),
            P("grp", "tp"),
            P("tp"),
            P(),
        ),
        out_specs=(
            P(("grp", "sp"), None, None, "tp"),
            P(("grp", "sp"), None, None, "tp"),
            P("grp", "tp"),
        ),
        check_vma=False,
    )
```
